32 devices in a mesh: grp: 2 (over y), fs: 4 (over z), tp: 4 (over x, core).
Axes of the slice: x: 2, y: 2, z: 4, core: 2. Of those that a mesh axis runs over, the one named last changes fastest.
Arguments:
- layer_input: bfloat16 [3072, 2048], P(('grp', 'fs'), 'tp'), parts along dimension 0, may hold values from -6 to 6
- first_gain: bfloat16 [1, 2048], P(None, 'tp'), may hold values from 0.099609375 to 1.8984375
- ffn_gate_w: bfloat16 [2048, 6144], P('fs', 'tp'), may hold values from -0.125 to 0.125
- ffn_up_w: bfloat16 [2048, 6144], P('fs', 'tp'), may hold values from -0.125 to 0.125
- ffn_down_w: bfloat16 [6144, 2048], P('tp', 'fs'), may hold values from -0.078125 to 0.078125
- mixer_gain: bfloat16 [1, 2048], P(None, 'tp'), may hold values from 0.099609375 to 1.8984375
- pool_in_w: bfloat16 [2048, 1024], P('fs', 'tp'), may hold values from -0.125 to 0.125
- mixer_gate_w: bfloat16 [2048, 2048], P('fs', 'tp'), may hold values from -0.125 to 0.125
- group_mix_w: bfloat16 [8, 128, 128], P('tp'), may hold values from -0.5 to 0.5
- pool_scale: float32 [1, 1024], P(None, 'tp'), may hold values from 0.1 to 1.9
- mixer_out_w: bfloat16 [1024, 2048], P('tp', 'fs'), may hold values from -0.1875 to 0.1875
- second_gain: bfloat16 [1, 2048], P(None, 'tp'), may hold values from 0.099609375 to 1.8984375
Outputs:
- layer_output: bfloat16 [3072, 2048], P(('grp', 'fs'), 'tp'), parts along dimension 0
The draws below stay inside these ranges and needn't reach their ends.
There are 2 independent parts, one for each index of `grp`. The reference program is written for one: setup_inputs(seed, part) draws one part's arguments, and reference() takes and returns one part's arrays. A program takes and returns all parts, laid end to end along the dimension named above; an argument that names none is the same for every part. Nothing has to cross between parts.
All inputs are finite; a program needn't handle non-finite values.
Results may differ from the reference program's by a relative error of at most 0.015.
Values may be sent and summed in bfloat16 or wider, within the bound.
A program may use at most 64 MiB of HBM per device.

```python
import jax
import jax.numpy as jnp
from jax import lax

D = 2048
FF = 6144
BW = 1024
GW = 128
GROUPS = 8
TOK_DEV = 384
TOKENS = 1536
N_FS = 4
N_TP = 4


def steps_of(key, dims, split, low, top_value):
    factor_of = 1.0
    for position, shards_of in split:
        draws = jax.random.uniform(jax.random.fold_in(jax.random.fold_in(key, 6), position), (shards_of,), jnp.float32, low / len(split), top_value / len(split))
        factor_of = factor_of * jnp.repeat(jnp.exp(draws), dims[position] // shards_of).reshape((-1,) + (1,) * (len(dims) - 1 - position))
    return factor_of


def noise(rng, extent, scale, bound, shards=(), kind=jnp.bfloat16):
    drawn = jax.random.normal(rng, extent, jnp.float32) * scale
    if len(shards) > 0:
        drawn = steps_of(rng, extent, shards, -0.22, 0.18) * drawn
    return jnp.clip(drawn, min=-bound, max=bound).astype(kind)


def setup_inputs(seed: int = 0, part: int = 0) -> dict:
    splits = jax.random.split(jax.random.key(seed), 13)
    part_keys = jax.random.split(jax.random.fold_in(splits[12], part), 13)
    layer_input = noise(part_keys[0], (TOKENS, D), 1.0, 6.0, ((0, 4), (1, 4)))
    first_gain = jnp.clip(1.0 + 0.18 * jax.random.normal(splits[1], (1, D), jnp.float32), 0.099609375, 1.8984375).astype(jnp.bfloat16)
    ffn_gate_w = noise(splits[2], (D, FF), D ** -0.5, 0.125, ((0, 4), (1, 4)))
    ffn_up_w = noise(splits[3], (D, FF), D ** -0.5, 0.125, ((0, 4), (1, 4)))
    ffn_down_w = noise(splits[4], (FF, D), FF ** -0.5, 0.078125, ((0, 4), (1, 4)))
    mixer_gain = jnp.clip(1.0 + 0.18 * jax.random.normal(splits[5], (1, D), jnp.float32), 0.099609375, 1.8984375).astype(jnp.bfloat16)
    pool_in_w = noise(splits[6], (D, BW), D ** -0.5, 0.125, ((0, 4), (1, 4)))
    mixer_gate_w = noise(splits[7], (D, D), D ** -0.5, 0.125, ((0, 4), (1, 4)))
    group_mix_w = noise(splits[8], (GROUPS, GW, GW), GW ** -0.5, 0.5, ((0, 4),))
    pool_scale = jnp.clip(1.0 + 0.18 * jax.random.normal(splits[9], (1, BW), jnp.float32), 0.1, 1.9)
    mixer_out_w = noise(splits[10], (BW, D), BW ** -0.5, 0.1875, ((0, 4), (1, 4)))
    second_gain = jnp.clip(1.0 + 0.18 * jax.random.normal(splits[11], (1, D), jnp.float32), 0.099609375, 1.8984375).astype(jnp.bfloat16)
    return dict(layer_input=layer_input, first_gain=first_gain, ffn_gate_w=ffn_gate_w, ffn_up_w=ffn_up_w, ffn_down_w=ffn_down_w, mixer_gain=mixer_gain, pool_in_w=pool_in_w, mixer_gate_w=mixer_gate_w, group_mix_w=group_mix_w, pool_scale=pool_scale, mixer_out_w=mixer_out_w, second_gain=second_gain)


def norm_rows(values, gain):
    widened = values.astype(jnp.float32)
    scaled = (widened * gain.astype(jnp.float32)).astype(jnp.bfloat16)
    factor = lax.rsqrt(lax.optimization_barrier(jnp.mean(widened * widened, axis=1, keepdims=True)) + 1e-06)
    return (scaled, factor)

def block_sum(left, right):
    width = left.shape[1] // N_TP
    total = jnp.zeros((left.shape[0], right.shape[1]), jnp.float32)
    for block in range(N_TP):
        partial_value = jnp.dot(left[:, block * width:(block + 1) * width], right[block * width:(block + 1) * width], preferred_element_type=jnp.float32)
        rounded = lax.optimization_barrier(partial_value.astype(jnp.bfloat16))
        total = total + rounded.astype(jnp.float32)
    return total

def feed_forward(values, gain, ffn_gate_w, ffn_up_w, ffn_down_w):
    scaled, factor = norm_rows(values, gain)
    gate_pre = factor * jnp.dot(scaled, ffn_gate_w, preferred_element_type=jnp.float32)
    up_pre = factor * jnp.dot(scaled, ffn_up_w, preferred_element_type=jnp.float32)
    hidden = (jax.nn.silu(gate_pre) * up_pre).astype(jnp.bfloat16)
    return block_sum(hidden, ffn_down_w)

def reference(layer_input, first_gain, ffn_gate_w, ffn_up_w, ffn_down_w, mixer_gain, pool_in_w, mixer_gate_w, group_mix_w, pool_scale, mixer_out_w, second_gain):
    first = (layer_input.astype(jnp.float32) + 0.5 * feed_forward(layer_input, first_gain, ffn_gate_w, ffn_up_w, ffn_down_w)).astype(jnp.bfloat16)
    scaled, factor = norm_rows(first, mixer_gain)
    pool_pre = (factor * jnp.dot(scaled, pool_in_w, preferred_element_type=jnp.float32)).astype(jnp.bfloat16)
    gate_logit = factor * jnp.dot(scaled, mixer_gate_w, preferred_element_type=jnp.float32)
    values = pool_pre.astype(jnp.float32).reshape(N_FS, TOK_DEV, GROUPS, GW)
    running = jnp.cumsum(values, axis=1)
    positions = jnp.arange(TOK_DEV, dtype=jnp.int32)
    windows = 2 ** (1 + jnp.arange(GROUPS, dtype=jnp.int32) % 4)
    chosen = jnp.zeros_like(values)
    for span in (2, 4, 8, 16):
        lagged = jnp.pad(running, ((0, 0), (span, 0), (0, 0), (0, 0)))[:, :TOK_DEV]
        counts = jnp.minimum(positions + 1, span).astype(jnp.float32)[None, :, None, None]
        means = (running - lagged) / counts
        chosen = jnp.where((windows == span)[None, None, :, None], means, chosen)
    trail = (chosen - values).astype(jnp.bfloat16)
    mixed = jnp.einsum('ntgc,gcd->ntgd', trail.astype(jnp.float32), group_mix_w.astype(jnp.float32))
    pooled = (mixed.reshape(TOKENS, BW) * pool_scale).astype(jnp.bfloat16)
    lifted = block_sum(pooled, mixer_out_w)
    second = (first.astype(jnp.float32) + jax.nn.sigmoid(gate_logit) * lifted).astype(jnp.bfloat16)
    result = second.astype(jnp.float32) + 0.5 * feed_forward(second, second_gain, ffn_gate_w, ffn_up_w, ffn_down_w)
    return result.astype(jnp.bfloat16)
```

```python
import functools

import jax
import jax.numpy as jnp
from jax import lax
from jax.experimental import pallas as pl
from jax.experimental.pallas import tpu as pltpu
from jax.sharding import PartitionSpec as P

MESH = pl.DeviceIdType.MESH
F32 = jnp.float32
BF16 = jnp.bfloat16
scope = jax.named_scope
GAIN_ROWS = 16


def ceil_pieces(rows, wanted):
    while rows % (wanted * 16) != 0:
        wanted -= 1
    return wanted


def layer_kernel(
    sizes,
    inputs,
    gain_rows,
    gate_w,
    up_w,
    down_w,
    pool_w,
    mgate_w,
    mout_w,
    mix_w,
    scale_w,
    out,
    gate_all,
    up_all,
    down_all,
    pool_all,
    mgate_all,
    mout_all,
    input_all,
    gain_all,
    value_all,
    scaled,
    factor,
    hidden,
    pooled,
    logit,
    parts,
    sums,
    mate_out,
    mate_in,
    mate_top,
    local_sem,
    z_recv,
    y_recv,
    z_send,
    y_send,
    v_send,
    v_relay,
    v_recv,
    g_send,
    g_relay,
    g_recv,
    s_send,
    s_recv,
    m_send,
    m_recv,
):
    grps, planes, tps, mates, piece_counts = sizes
    g = lax.axis_index("grp")
    f = lax.axis_index("fs")
    tp = lax.axis_index("tp")
    rows, width = out.shape
    chips = tps // 2
    chip, core = tp // 2, tp % 2
    partner = chip * 2 + (core + 1) % 2
    twins = [((chip + i) % chips) * 2 + core for i in range(1, chips)]
    crosses = [((chip + i) % chips) * 2 + (core + 1) % 2 for i in range(1, chips)]
    peers = twins + [partner]
    other_grps = [(g + d) % grps for d in range(1, grps)]
    side = f % mates
    mate = f + 1 - 2 * side

    barrier = pltpu.get_barrier_semaphore()
    for peer in peers:
        pl.semaphore_signal(barrier, inc=1, device_id={"tp": peer}, device_id_type=MESH)
    for other in other_grps:
        pl.semaphore_signal(barrier, inc=1, device_id={"grp": other}, device_id_type=MESH)

    @pl.when(f > 0)
    def _():
        pl.semaphore_signal(barrier, inc=1, device_id={"fs": f - 1}, device_id_type=MESH)

    @pl.when(f < planes - 1)
    def _():
        pl.semaphore_signal(barrier, inc=1, device_id={"fs": f + 1}, device_id_type=MESH)

    inner = jnp.where(f > 0, 1, 0) + jnp.where(f < planes - 1, 1, 0)
    pl.semaphore_wait(barrier, len(peers) + len(other_grps) + inner)

    def gathered(lane):
        return input_all if lane == 0 else value_all.at[lane - 1]

    half_rows = rows // 2
    halves = (slice(0, half_rows), slice(half_rows, rows))

    def value_copy(lane, block, half, peer=None, source=None):
        relay = source is not None
        ref = inputs if lane == 0 and not relay else gathered(source if relay else lane).at[block]
        target = 1 if peer is None else 0
        if relay:
            send_sem = v_relay.at[lane, half, block, target]
        else:
            send_sem = v_send.at[lane, half, tps if peer is None else peer]
        to = lane if peer is not None else lane + 3 if lane == 0 else 4
        return pltpu.make_async_remote_copy(
            src_ref=ref.at[halves[half], :],
            dst_ref=gathered(to).at[block, halves[half], :],
            send_sem=send_sem,
            recv_sem=v_recv.at[to, half, block],
            device_id={"fs": mate} if peer is None else {"tp": peer},
            device_id_type=MESH,
        )

    def gain_copy(block, peer, relay=False):
        return pltpu.make_async_remote_copy(
            src_ref=gain_all.at[block] if relay else gain_rows,
            dst_ref=gain_all.at[block],
            send_sem=g_relay.at[block] if relay else g_send.at[peer],
            recv_sem=g_recv.at[block],
            device_id={"tp": peer},
            device_id_type=MESH,
        )

    def mate_sum_copy(ffn, block, top=False):
        if top:
            source, target = mate_out.at[ffn, halves[0], :], mate_top.at[ffn]
        else:
            target = mate_in.at[ffn, block]
            source = parts.at[ffn_lanes(ffn)[-1], block, halves[1], :]
        number = tps if top else block
        return pltpu.make_async_remote_copy(
            src_ref=source,
            dst_ref=target,
            send_sem=m_send.at[ffn, number],
            recv_sem=m_recv.at[ffn, number],
            device_id={"fs": mate},
            device_id_type=MESH,
        )

    def own_sum_copy(ffn):
        return pltpu.make_async_remote_copy(
            src_ref=mate_out.at[ffn, halves[1], :],
            dst_ref=mate_in.at[ffn, tp],
            send_sem=m_send.at[ffn, tp],
            recv_sem=m_recv.at[ffn, tp],
            device_id={"fs": mate},
            device_id_type=MESH,
        )

    def sum_copy(lane, block, slot, peer, half=None):
        span = slice(0, rows) if half is None else halves[half]
        number = 0 if half is None else half
        return pltpu.make_async_remote_copy(
            src_ref=parts.at[lane, block, span, :],
            dst_ref=sums.at[lane, slot, span, :],
            send_sem=s_send.at[lane, number, block],
            recv_sem=s_recv.at[lane, number, slot],
            device_id={"tp": peer},
            device_id_type=MESH,
        )

    weights = (
        (gate_w, gate_all, "columns"),
        (up_w, up_all, "columns"),
        (down_w, down_all, "rows"),
        (pool_w, pool_all, "plain"),
        (mgate_w, mgate_all, "plain"),
        (mout_w, mout_all, "stacked"),
    )
    pieces = []
    for numbers in ((0, 1), (2,), (3,), (4,), (5,)):
        for part in range(piece_counts[numbers[0]]):
            for number in numbers:
                for share in range(mates) if number < 3 else (None,):
                    pieces.append((number, share, part))
    share_units = down_w.shape[0] // mates

    def span_of(piece, grp):
        number, share, part = pieces[piece]
        kind = weights[number][2]
        tall = share_units if kind == "rows" else weights[number][0].shape[0]
        half = tall // grps
        size = half // piece_counts[number]
        offset = share * share_units if kind == "rows" else 0
        return offset + grp * half + part * size, size

    def place(piece, plane, grp):
        number, share, part = pieces[piece]
        shard, whole, kind = weights[number]
        start, size = span_of(piece, grp)
        if kind in ("rows", "stacked"):
            return whole.at[plane, pl.ds(pl.multiple_of(start, 16), size), :]
        span = pl.ds(pl.multiple_of(plane * shard.shape[0] + start, 16), size)
        if kind == "columns":
            return whole.at[share, span, :]
        return whole.at[span, :]

    def own_place(piece):
        number, share, part = pieces[piece]
        shard, whole, kind = weights[number]
        start, size = span_of(piece, g)
        span = pl.ds(pl.multiple_of(start, 16), size)
        if kind == "columns":
            return shard.at[span, share * share_units : (share + 1) * share_units]
        return shard.at[span, :]

    def ends(piece):
        share = pieces[piece][1]
        if share is None:
            return 0, planes - 1
        return share, planes - mates + share

    def wanted(piece):
        share = pieces[piece][1]
        return True if share is None else side == share

    def z_copy(piece, plane, step, own=False):
        spot = place(piece, plane, g)
        return pltpu.make_async_remote_copy(
            src_ref=own_place(piece) if own else spot,
            dst_ref=spot,
            send_sem=z_send.at[piece, planes if own and step < 0 else plane],
            recv_sem=z_recv.at[piece, plane],
            device_id={"fs": f + step},
            device_id_type=MESH,
        )

    def y_copy(piece, plane, number, source, arriving=False):
        spot = place(piece, plane, source)
        there = number if arriving else grps - 2 - number
        return pltpu.make_async_remote_copy(
            src_ref=spot,
            dst_ref=spot,
            send_sem=y_send.at[piece, plane, number],
            recv_sem=y_recv.at[piece, plane, there],
            device_id={"grp": other_grps[number]},
            device_id_type=MESH,
        )

    def send_own(piece, early=None):
        low, high = ends(piece)
        up, down = f < high, f > low
        if pieces[piece][0] > 2:
            outward_up, outward_down = f >= planes // 2, f < planes // 2
            up = up & (outward_up if early else jnp.logical_not(outward_up))
            down = down & (outward_down if early else jnp.logical_not(outward_down))

        @pl.when(up)
        def _():
            z_copy(piece, f, 1, own=True).start()

        @pl.when(down)
        def _():
            z_copy(piece, f, -1, own=True).start()

    def take(piece, hop):
        low, high = ends(piece)

        @pl.when((f >= hop) & (f <= high))
        def _():
            z_copy(piece, f - hop, -1).wait_recv()

            @pl.when(f < high)
            def _():
                z_copy(piece, f - hop, 1).start()

            @pl.when(wanted(piece))
            def _():
                for number in range(len(other_grps)):
                    y_copy(piece, f - hop, number, g).start()

        @pl.when((f + hop < planes) & (f >= low))
        def _():
            z_copy(piece, f + hop, 1).wait_recv()

            @pl.when(f > low)
            def _():
                z_copy(piece, f + hop, -1).start()

            @pl.when(wanted(piece))
            def _():
                for number in range(len(other_grps)):
                    y_copy(piece, f + hop, number, g).start()

    def advance(until):
        while clock[0] < until:
            step = clock[0]
            if step + ahead < len(pieces):
                send_own(step + ahead)
            if step in early_at:
                send_own(early_at[step], early=True)
            for hop in range(planes - 1, 0, -1):
                piece = step - (hop - 1) * lag
                if 0 <= piece < len(pieces):
                    take(piece, hop)
            clock[0] += 1

    def after(piece):
        return piece + 1 + (planes - 2) * lag

    def sent(piece):
        low, high = ends(piece)

        @pl.when(f < high)
        def _():
            z_copy(piece, f, 1, own=True).wait_send()

        @pl.when(f > low)
        def _():
            z_copy(piece, f, -1, own=True).wait_send()

        for hop in range(1, planes):

            @pl.when((f >= hop) & (f <= high))
            def _():
                @pl.when(f < high)
                def _():
                    z_copy(piece, f - hop, 1).wait_send()

                @pl.when(wanted(piece))
                def _():
                    for number in range(len(other_grps)):
                        y_copy(piece, f - hop, number, g).wait_send()

            @pl.when((f + hop < planes) & (f >= low))
            def _():
                @pl.when(f > low)
                def _():
                    z_copy(piece, f + hop, -1).wait_send()

                @pl.when(wanted(piece))
                def _():
                    for number in range(len(other_grps)):
                        y_copy(piece, f + hop, number, g).wait_send()

    def of(*numbers):
        return [p for p, piece in enumerate(pieces) if piece[0] in numbers]

    clock = [0]
    ahead = 3
    mixer_pieces = of(3, 4, 5)
    early_at = {8 * mixer_pieces[0] // 24 + i: p for i, p in enumerate(mixer_pieces)}
    lag = 1

    def arrive(*numbers):
        for number in numbers:
            local_copy(number).wait()
        for piece in of(*numbers):

            @pl.when(wanted(piece))
            def _():
                for step in range(1, planes):
                    plane = (f + step) % planes
                    for number, other in enumerate(other_grps):
                        y_copy(piece, plane, number, other, arriving=True).wait_recv()

    def local_copy(number):
        shard, whole, kind = weights[number]
        tall = shard.shape[0]
        span = pl.ds(pl.multiple_of(f * tall, 16), tall)
        if kind == "columns":
            mine = pl.ds(pl.multiple_of(side * share_units, 128), share_units)
            shard, spot = shard.at[:, mine], whole.at[side, span, :]
        elif kind == "rows":
            mine = pl.ds(pl.multiple_of(side * share_units, 16), share_units)
            shard, spot = shard.at[mine, :], whole.at[f, mine, :]
        elif kind == "stacked":
            spot = whole.at[f]
        else:
            spot = whole.at[span, :]
        return pltpu.make_async_copy(shard, spot, local_sem.at[number])

    def local_input():
        return pltpu.make_async_copy(inputs, input_all.at[tp], local_sem.at[len(weights)])

    def local_gain():
        return pltpu.make_async_copy(gain_rows, gain_all.at[tp], local_sem.at[len(weights) + 1])

    row_tile = [t for t in (96, 64, 32, 16) if rows % t == 0][0]

    def spread(lane, half, with_mate=False):
        for peer in peers:
            value_copy(lane, tp, half, peer).start()
        if with_mate and mates > 1:
            value_copy(lane, tp, half).start()

    def landed(lane, block, half):
        value_copy(lane, block, half, partner).wait_recv()

    def relay_values(lane, half, with_mate=False):
        for twin in twins:
            landed(lane, twin, half)
            value_copy(lane, twin, half, partner, source=lane).start()
            if with_mate and mates > 1 and half == 1:
                value_copy(lane, twin, half, source=lane).start()

    def relay_mate(lane, half):
        landed(lane, tp, half)
        for peer in peers if half == 0 else [partner]:
            value_copy(lane, tp, half, peer, source=lane).start()

    def relay_mate_twins(lane):
        for half in range(2):
            for twin in twins:
                landed(lane, twin, half)
                value_copy(lane, twin, half, partner, source=lane).start()

    def gather_start(lane):
        for half in range(2):
            spread(lane, half, with_mate=True)

    def gather_relay(lane, mate_lane):
        relay_values(lane, 0)
        if mates > 1:
            relay_mate(mate_lane, 0)
        relay_values(lane, 1, with_mate=True)
        if mates > 1:
            relay_mate(mate_lane, 1)

    def value_sent(lane, with_mate=False):
        for half in range(2):
            for peer in peers:
                value_copy(lane, tp, half, peer).wait_send()
            for twin in twins:
                value_copy(lane, twin, half, partner, source=lane).wait_send()
            if with_mate and mates > 1:
                value_copy(lane, tp, half).wait_send()
                if half == 1:
                    for twin in twins:
                        value_copy(lane, twin, half, source=lane).wait_send()

    def mate_sent(lane):
        for half in range(2):
            for peer in peers if half == 0 else [partner]:
                value_copy(lane, tp, half, peer, source=lane).wait_send()
            for twin in twins:
                value_copy(lane, twin, half, partner, source=lane).wait_send()

    def scale_values(lane, slot, gain):
        for half in range(2):
            for block in [partner] + crosses:
                landed(lane, block, half)
        ref = gathered(lane)

        def body(step, carry):
            start = pl.multiple_of(step * row_tile, row_tile)
            span = pl.ds(start, row_tile)
            target = pl.ds(slot * rows + start, row_tile)
            total = jnp.zeros((row_tile, 1), F32)
            for t in range(tps):
                gains = gain_all[t].astype(F32)
                value = ref[t, span, :].astype(F32)
                total = total + jnp.sum(value * value, axis=1, keepdims=True)
                scaled[target, t * width : (t + 1) * width] = (
                    value * gains[gain : gain + 1]
                ).astype(BF16)
            factor[target, :] = lax.rsqrt(total / (tps * width) + 1e-06)
            return carry

        lax.fori_loop(0, rows // row_tile, body, 0)

    def hidden_units(slot):
        units = hidden.shape[1]
        tile = 256 if units % 256 == 0 else 128
        mine = slice(slot * rows, (slot + 1) * rows)

        def body(step, carry):
            span = pl.ds(pl.multiple_of(step * tile, tile), tile)
            gate = factor[mine, :] * jnp.dot(
                scaled[mine, :], gate_all[side, :, span], preferred_element_type=F32
            )
            up = factor[mine, :] * jnp.dot(
                scaled[mine, :], up_all[side, :, span], preferred_element_type=F32
            )
            hidden[mine, span] = (jax.nn.silu(gate) * up).astype(BF16)
            return carry

        lax.fori_loop(0, units // tile, body, 0)

    ratio = planes // tps
    block_width = width // ratio

    def product(left, right_of, lane, slot, block_of):
        for piece in range(ratio):
            parts[lane, block_of, :, piece * block_width : (piece + 1) * block_width] = jnp.dot(
                left[slot * rows : (slot + 1) * rows, :],
                right_of(block_of * ratio + piece),
                preferred_element_type=F32,
            ).astype(BF16)

    def join_cross(lane, twin, cross):
        sum_copy(lane, cross, cross, partner).wait_recv()
        parts[lane, twin] = (
            parts[lane, twin].astype(F32) + sums[lane, cross].astype(F32)
        ).astype(BF16)

    def project_mixer(lane):
        left, right_of = pooled, lambda plane: mout_all[plane]
        for twin, cross in zip(twins, crosses):
            product(left, right_of, lane, 0, cross)
            sum_copy(lane, cross, twin, partner).start()
        for twin, cross in zip(twins, crosses):
            product(left, right_of, lane, 0, twin)
            join_cross(lane, twin, cross)
            for half in range(2):
                sum_copy(lane, twin, tp, twin, half).start()
        product(left, right_of, lane, 0, partner)
        sum_copy(lane, partner, tp, partner).start()
        product(left, right_of, lane, 0, tp)

    def sum_sent(lane, half_only=None):
        for block in crosses + [partner]:
            sum_copy(lane, block, tp, partner).wait_send()
        for twin in twins:
            for half in range(2) if half_only is None else [half_only]:
                sum_copy(lane, twin, tp, twin, half).wait_send()

    def down_of(plane):
        return down_all[plane, pl.ds(pl.multiple_of(side * share_units, 16), share_units), :]

    def ffn_lanes(ffn):
        return [ffn * (mates + 1) + slot for slot in range(mates)]

    def project_ffn(ffn):
        lanes = ffn_lanes(ffn)
        order = range(mates - 1, -1, -1)
        for slot in order:
            for twin, cross in zip(twins, crosses):
                product(hidden, down_of, lanes[slot], slot, cross)
                sum_copy(lanes[slot], cross, twin, partner).start()
        for slot in order:
            for twin, cross in zip(twins, crosses):
                product(hidden, down_of, lanes[slot], slot, twin)
                join_cross(lanes[slot], twin, cross)
                if slot > 0:
                    mate_sum_copy(ffn, twin).start()
                sum_copy(lanes[slot], twin, tp, twin, 0).start()
                if mates == 1:
                    sum_copy(lanes[slot], twin, tp, twin, 1).start()
        for slot in order:
            product(hidden, down_of, lanes[slot], slot, partner)
            sum_copy(lanes[slot], partner, tp, partner).start()
        for slot in order:
            product(hidden, down_of, lanes[slot], slot, tp)

    def half_total(lane, half, joined=False):
        total = parts[lane, tp, halves[half], :].astype(F32)
        if not joined:
            total = total + sums[lane, partner, halves[half], :].astype(F32)
        return total

    def add_twins(lane, half, total):
        for twin in twins:
            sum_copy(lane, twin, twin, partner, half).wait_recv()
            total = total + sums[lane, twin, halves[half], :].astype(F32)
        return total

    def exchange_ffn(ffn):
        lanes = ffn_lanes(ffn)
        if mates > 1:
            sum_copy(lanes[1], partner, partner, partner).wait_recv()
            mate_out[ffn, halves[1], :] = half_total(lanes[1], 1).astype(BF16)
            own_sum_copy(ffn).start()
            for twin in twins:
                mate_sum_copy(ffn, twin).wait_recv()
                parts[lanes[0], twin, halves[1], :] = (
                    parts[lanes[0], twin, halves[1], :].astype(F32)
                    + mate_in[ffn, twin].astype(F32)
                ).astype(BF16)
                sum_copy(lanes[0], twin, tp, twin, 1).start()
            mate_out[ffn, halves[0], :] = add_twins(
                lanes[1], 0, half_total(lanes[1], 0)
            ).astype(BF16)
            mate_sum_copy(ffn, tp, top=True).start()
        sum_copy(lanes[0], partner, partner, partner).wait_recv()

    def ffn_total(ffn, half):
        lane = ffn_lanes(ffn)[0]
        total = add_twins(lane, half, half_total(lane, half))
        if mates > 1 and half == 0:
            mate_sum_copy(ffn, tp, top=True).wait_recv()
            total = total + mate_top[ffn].astype(F32)
        elif mates > 1:
            own_sum_copy(ffn).wait_recv()
            total = total + mate_in[ffn, tp].astype(F32)
        return total

    def ffn_sent(ffn):
        lanes = ffn_lanes(ffn)
        sum_sent(lanes[0])
        if mates > 1:
            sum_sent(lanes[1], half_only=0)
            own_sum_copy(ffn).wait_send()
            mate_sum_copy(ffn, tp, top=True).wait_send()
            for twin in twins:
                mate_sum_copy(ffn, twin).wait_send()

    local_input().start()
    local_gain().start()
    for half in range(2):
        spread(0, half)
    for peer in peers:
        gain_copy(tp, peer).start()
    for piece in range(ahead):
        send_own(piece)
    for number in range(len(weights)):
        local_copy(number).start()
    with scope("begin"):
        advance(1)
    local_input().wait()
    local_gain().wait()
    with scope("input_own"):
        for twin in twins:
            gain_copy(twin, partner).wait_recv()
            gain_copy(twin, partner, relay=True).start()
        for block in [partner] + crosses:
            gain_copy(block, partner).wait_recv()
        for half in range(2):
            relay_values(0, half)
        scale_values(0, 0, 0)
    with scope("early"):
        if mates > 1:
            value_copy(0, tp, 0).start()
        advance(2)
        if mates > 1:
            value_copy(0, tp, 1).start()
        advance(4)
    with scope("input_mate"):
        if mates > 1:
            for twin in twins:
                value_copy(0, twin, 1, source=0).start()
            relay_mate(3, 0)
            relay_mate(3, 1)
        advance(6)
        if mates > 1:
            relay_mate_twins(3)
    with scope("early2"):
        advance(7)
    with scope("mate_scale"):
        if mates > 1:
            scale_values(3, 1, 0)
    first_last, down_last = of(0, 1)[-1], of(2)[-1]
    with scope("gate_up"):
        advance(after(first_last) + 2)
    with scope("gate_up_y"):
        arrive(0, 1)
    for slot in range(mates):
        with scope(f"hidden{slot}"):
            hidden_units(slot)
        with scope(f"step{slot}"):
            advance(min(clock[0] + 2, after(down_last)))
    with scope("down"):
        advance(after(down_last))
    with scope("down_y"):
        arrive(2)
    with scope("project0"):
        project_ffn(0)
    with scope("mix_pool"):
        advance(after(of(3)[-1]))
    with scope("exchange0"):
        exchange_ffn(0)
    with scope("mix_gate"):
        advance(after(of(4)[0]))
    with scope("first"):
        for half, span in enumerate(halves):
            value_all[0, tp, span, :] = (
                input_all[tp, span, :].astype(F32) + 0.5 * ffn_total(0, half)
            ).astype(BF16)
            spread(1, half)
    with scope("mix_rest"):
        advance(after(len(pieces) - 1))
    with scope("sent1"):
        value_sent(0, with_mate=True)
        for peer in peers:
            gain_copy(tp, peer).wait_send()
        for twin in twins:
            gain_copy(twin, partner, relay=True).wait_send()
        if mates > 1:
            mate_sent(3)
        for piece in of(0):
            sent(piece)
    with scope("relay1"):
        for half in range(2):
            relay_values(1, half)
    with scope("scale1"):
        scale_values(1, 0, 1)
    with scope("mix_y"):
        arrive(3, 4)
    groups, group_width = mix_w.shape[0], mix_w.shape[1]
    with scope("pool"):
        mixed_rows = slice(0, rows)
        pool_pre = (
            factor[mixed_rows, :]
            * jnp.dot(scaled[mixed_rows, :], pool_all[...], preferred_element_type=F32)
        ).astype(BF16)
        position = lax.broadcasted_iota(jnp.int32, (rows, group_width), 0)
        for group in range(groups):
            span = slice(group * group_width, (group + 1) * group_width)
            value = pool_pre[:, span].astype(F32)
            kind = (tp * groups + group) % 4
            running = value
            chosen = jnp.zeros_like(value)
            for level in range(4):
                lag = 2**level
                running = running + jnp.where(
                    position >= lag, pltpu.roll(running, lag, axis=0), 0.0
                )
                counts = jnp.minimum(position + 1, 2 * lag).astype(F32)
                chosen = jnp.where(kind == level, running / counts, chosen)
            trail = (chosen - value).astype(BF16)
            mixed = jnp.dot(trail, mix_w[group], preferred_element_type=F32)
            pooled[:, span] = (mixed * scale_w[:, span]).astype(BF16)
    with scope("mix_y2"):
        arrive(5)
    with scope("project1"):
        project_mixer(mates)
    with scope("logit"):
        logit[...] = factor[mixed_rows, :] * jnp.dot(
            scaled[mixed_rows, :], mgate_all[...], preferred_element_type=F32
        )
        logit[...] = jax.nn.sigmoid(logit[...])
    with scope("sent2"):
        ffn_sent(0)
        value_sent(1)
    with scope("second"):
        sum_copy(mates, partner, partner, partner).wait_recv()
        for half, span in enumerate(halves):
            value_all[1, tp, span, :] = (
                value_all[0, tp, span, :].astype(F32)
                + logit[span, :] * add_twins(mates, half, half_total(mates, half))
            ).astype(BF16)
            spread(2, half, with_mate=True)
    with scope("sent3"):
        for piece in of(1, 2):
            sent(piece)
    with scope("relay2"):
        gather_relay(2, 4)
    with scope("scale2"):
        scale_values(2, 0, 2)
    with scope("hidden2_0"):
        hidden_units(0)
    if mates > 1:
        with scope("relay4"):
            relay_mate_twins(4)
            for piece in of(3, 4, 5):
                sent(piece)
        with scope("scale4"):
            scale_values(4, 1, 2)
        with scope("hidden2_1"):
            hidden_units(1)
    with scope("project2"):
        project_ffn(1)
    with scope("exchange2"):
        exchange_ffn(1)
    with scope("sent4"):
        sum_sent(mates)
        value_sent(2, with_mate=True)
        if mates > 1:
            mate_sent(4)
        else:
            for piece in of(3, 4, 5):
                sent(piece)
    with scope("final"):
        for half, span in enumerate(halves):
            out[span, :] = (
                value_all[1, tp, span, :].astype(F32) + 0.5 * ffn_total(1, half)
            ).astype(BF16)
    with scope("sent5"):
        ffn_sent(1)


def per_device(
    grps,
    planes,
    tps,
    layer_input,
    first_gain,
    ffn_gate_w,
    ffn_up_w,
    ffn_down_w,
    mixer_gain,
    pool_in_w,
    mixer_gate_w,
    group_mix_w,
    pool_scale,
    mixer_out_w,
    second_gain,
):
    rows, width = layer_input.shape
    features = width * tps
    gains = jnp.concatenate([first_gain, mixer_gain, second_gain], axis=0)
    gain_rows = jnp.pad(gains, ((0, GAIN_ROWS - 3), (0, 0)))
    units = ffn_gate_w.shape[1]
    channels = pool_in_w.shape[1]
    mates = 2 if planes % 2 == 0 else 1
    fine = max(8 // planes, 1)
    wanted = (fine, fine, fine, max(fine // 2, 1), fine, max(fine // 2, 1))
    shards = (ffn_gate_w, ffn_up_w, ffn_down_w, pool_in_w, mixer_gate_w, mixer_out_w)
    talls = [shard.shape[0] // grps for shard in shards]
    talls[2] //= mates
    piece_counts = tuple(ceil_pieces(tall, count) for tall, count in zip(talls, wanted))
    n = mates * sum(piece_counts[:3]) + sum(piece_counts[3:])
    lanes = 2 * mates + 1
    dma = pltpu.SemaphoreType.DMA
    whole = pl.BlockSpec(memory_space=pltpu.VMEM)
    remote = pl.BlockSpec(memory_space=pl.ANY)
    return pl.pallas_call(
        functools.partial(layer_kernel, (grps, planes, tps, mates, piece_counts)),
        out_shape=jax.ShapeDtypeStruct((rows, width), BF16),
        in_specs=[remote] * 8 + [whole] * 2,
        out_specs=whole,
        scratch_shapes=[
            pltpu.VMEM((mates, features, units // mates), BF16),
            pltpu.VMEM((mates, features, units // mates), BF16),
            pltpu.VMEM((planes,) + ffn_down_w.shape, BF16),
            pltpu.VMEM((features, channels), BF16),
            pltpu.VMEM((features, width), BF16),
            pltpu.VMEM((planes,) + mixer_out_w.shape, BF16),
            pltpu.VMEM((tps, rows, width), BF16),
            pltpu.VMEM((tps, GAIN_ROWS, width), BF16),
            pltpu.VMEM((2 * mates, tps, rows, width), BF16),
            pltpu.VMEM((mates * rows, features), BF16),
            pltpu.VMEM((mates * rows, 1), F32),
            pltpu.VMEM((mates * rows, units // mates), BF16),
            pltpu.VMEM((rows, channels), BF16),
            pltpu.VMEM((rows, width), F32),
            pltpu.VMEM((lanes, tps, rows, width), BF16),
            pltpu.VMEM((lanes, tps, rows, width), BF16),
            pltpu.VMEM((2, rows, width), BF16),
            pltpu.VMEM((2, tps, rows // 2, width), BF16),
            pltpu.VMEM((2, rows // 2, width), BF16),
            dma((len(shards) + 2,)),
            dma((n, planes)),
            dma((n, planes, max(grps - 1, 1))),
            dma((n, planes + 1)),
            dma((n, planes, max(grps - 1, 1))),
            dma((5, 2, tps + 1)),
            dma((5, 2, tps, 2)),
            dma((5, 2, tps)),
            dma((tps,)),
            dma((tps,)),
            dma((tps,)),
            dma((lanes, 2, tps)),
            dma((lanes, 2, tps)),
            dma((2, tps + 1)),
            dma((2, tps + 1)),
        ],
        compiler_params=pltpu.CompilerParams(
            collective_id=0, has_side_effects=True, vmem_limit_bytes=60 * 1024 * 1024
        ),
    )(layer_input, gain_rows, *shards, group_mix_w, pool_scale)


def solution(mesh):
    return jax.shard_map(
        functools.partial(
            per_device, mesh.shape["grp"], mesh.shape["fs"], mesh.shape["tp"]
        ),
        mesh=mesh,
        in_specs=(
            P(("grp", "fs"), "tp"),
            P(None, "tp"),
            P("fs", "tp"),
            P("fs", "tp"),
            P("tp", "fs"),
            P(None, "tp"),
            P("fs", "tp"),
            P("fs", "tp"),
            P("tp", None, None),
            P(None, "tp"),
            P("tp", "fs"),
            P(None, "tp"),
        ),
        out_specs=P(("grp", "fs"), "tp"),
        check_vma=False,
    )
```

```python
import functools

import jax
import jax.numpy as jnp
from jax import lax
from jax.experimental import pallas as pl
from jax.experimental.pallas import tpu as pltpu
from jax.sharding import PartitionSpec as P

MESH = pl.DeviceIdType.MESH
F32 = jnp.float32
BF16 = jnp.bfloat16
scope = jax.named_scope
GAIN_ROWS = 16


def ceil_pieces(rows, wanted):
    while rows % (wanted * 16) != 0:
        wanted -= 1
    return wanted


def layer_kernel(
    sizes,
    inputs,
    first_gain,
    mixer_gain,
    second_gain,
    gate_w,
    up_w,
    down_w,
    pool_w,
    mgate_w,
    mout_w,
    mix_w,
    scale_w,
    out,
    gate_all,
    up_all,
    down_all,
    pool_all,
    mgate_all,
    mout_all,
    input_all,
    gain_all,
    value_all,
    scaled,
    factor,
    hidden,
    pooled,
    logit,
    parts,
    sums,
    mate_out,
    mate_in,
    mate_top,
    local_sem,
    z_recv,
    y_recv,
    z_send,
    y_send,
    v_send,
    v_relay,
    v_recv,
    g_send,
    g_recv,
    s_send,
    s_recv,
    m_send,
    m_recv,
):
    grps, planes, tps, mates, piece_counts = sizes
    g = lax.axis_index("grp")
    f = lax.axis_index("fs")
    tp = lax.axis_index("tp")
    rows, width = out.shape
    chips = tps // 2
    chip, core = tp // 2, tp % 2
    partner = chip * 2 + (core + 1) % 2
    twins = [((chip + i) % chips) * 2 + core for i in range(1, chips)]
    crosses = [((chip + i) % chips) * 2 + (core + 1) % 2 for i in range(1, chips)]
    peers = twins + [partner]
    other_grps = [(g + d) % grps for d in range(1, grps)]
    side = f % mates
    mate = f + 1 - 2 * side

    barrier = pltpu.get_barrier_semaphore()
    for peer in peers:
        pl.semaphore_signal(barrier, inc=1, device_id={"tp": peer}, device_id_type=MESH)
    for other in other_grps:
        pl.semaphore_signal(barrier, inc=1, device_id={"grp": other}, device_id_type=MESH)

    @pl.when(f > 0)
    def _():
        pl.semaphore_signal(barrier, inc=1, device_id={"fs": f - 1}, device_id_type=MESH)

    @pl.when(f < planes - 1)
    def _():
        pl.semaphore_signal(barrier, inc=1, device_id={"fs": f + 1}, device_id_type=MESH)

    inner = jnp.where(f > 0, 1, 0) + jnp.where(f < planes - 1, 1, 0)
    pl.semaphore_wait(barrier, len(peers) + len(other_grps) + inner)

    def gathered(lane):
        return input_all if lane == 0 else value_all.at[lane - 1]

    half_rows = rows // 2
    halves = (slice(0, half_rows), slice(half_rows, rows))

    def value_copy(lane, block, half, peer=None, source=None):
        relay = source is not None
        ref = inputs if lane == 0 and not relay else gathered(source if relay else lane).at[block]
        to = lane if peer is not None else lane + 3 if lane == 0 else 4
        return pltpu.make_async_remote_copy(
            src_ref=ref.at[halves[half], :],
            dst_ref=gathered(to).at[block, halves[half], :],
            send_sem=(v_relay if relay else v_send).at[lane],
            recv_sem=v_recv.at[to, half, block],
            device_id={"fs": mate} if peer is None else {"tp": peer},
            device_id_type=MESH,
        )

    def gain_copy(block, peer, relay=False):
        return pltpu.make_async_remote_copy(
            src_ref=gain_all.at[block],
            dst_ref=gain_all.at[block],
            send_sem=g_send,
            recv_sem=g_recv.at[block],
            device_id={"tp": peer},
            device_id_type=MESH,
        )

    def mate_sum_copy(ffn, block, top=False):
        if top:
            source, target = mate_out.at[ffn, halves[0], :], mate_top.at[ffn]
        else:
            target = mate_in.at[ffn, block]
            source = parts.at[ffn_lanes(ffn)[-1], block, halves[1], :]
        number = tps if top else block
        return pltpu.make_async_remote_copy(
            src_ref=source,
            dst_ref=target,
            send_sem=m_send.at[ffn],
            recv_sem=m_recv.at[ffn, number],
            device_id={"fs": mate},
            device_id_type=MESH,
        )

    def own_sum_copy(ffn):
        return pltpu.make_async_remote_copy(
            src_ref=mate_out.at[ffn, halves[1], :],
            dst_ref=mate_in.at[ffn, tp],
            send_sem=m_send.at[ffn],
            recv_sem=m_recv.at[ffn, tp],
            device_id={"fs": mate},
            device_id_type=MESH,
        )

    def sum_copy(lane, block, slot, peer, half=None):
        span = slice(0, rows) if half is None else halves[half]
        number = 0 if half is None else half
        return pltpu.make_async_remote_copy(
            src_ref=parts.at[lane, block, span, :],
            dst_ref=sums.at[lane, slot, span, :],
            send_sem=s_send.at[lane],
            recv_sem=s_recv.at[lane, number, slot],
            device_id={"tp": peer},
            device_id_type=MESH,
        )

    weights = (
        (gate_w, gate_all, "columns"),
        (up_w, up_all, "columns"),
        (down_w, down_all, "rows"),
        (pool_w, pool_all, "plain"),
        (mgate_w, mgate_all, "plain"),
        (mout_w, mout_all, "stacked"),
    )
    pieces = []
    for numbers in ((0, 1), (2,), (3,), (4,), (5,)):
        for part in range(piece_counts[numbers[0]]):
            for number in numbers:
                for share in range(mates) if number < 3 else (None,):
                    pieces.append((number, share, part))
    share_units = down_w.shape[0] // mates

    def span_of(piece, grp):
        number, share, part = pieces[piece]
        kind = weights[number][2]
        tall = share_units if kind == "rows" else weights[number][0].shape[0]
        half = tall // grps
        size = half // piece_counts[number]
        offset = share * share_units if kind == "rows" else 0
        return offset + grp * half + part * size, size

    def place(piece, plane, grp):
        number, share, part = pieces[piece]
        shard, whole, kind = weights[number]
        start, size = span_of(piece, grp)
        if kind in ("rows", "stacked"):
            return whole.at[plane, pl.ds(pl.multiple_of(start, 16), size), :]
        span = pl.ds(pl.multiple_of(plane * shard.shape[0] + start, 16), size)
        if kind == "columns":
            return whole.at[share, span, :]
        return whole.at[span, :]

    def own_place(piece):
        number, share, part = pieces[piece]
        shard, whole, kind = weights[number]
        start, size = span_of(piece, g)
        span = pl.ds(pl.multiple_of(start, 16), size)
        if kind == "columns":
            return shard.at[span, share * share_units : (share + 1) * share_units]
        return shard.at[span, :]

    def ends(piece):
        share = pieces[piece][1]
        if share is None:
            return 0, planes - 1
        return share, planes - mates + share

    def wanted(piece):
        share = pieces[piece][1]
        return True if share is None else side == share

    def z_copy(piece, plane, step, own=False):
        spot = place(piece, plane, g)
        return pltpu.make_async_remote_copy(
            src_ref=own_place(piece) if own else spot,
            dst_ref=spot,
            send_sem=z_send.at[piece],
            recv_sem=z_recv.at[piece, plane],
            device_id={"fs": f + step},
            device_id_type=MESH,
        )

    def y_copy(piece, plane, number, source, arriving=False):
        spot = place(piece, plane, source)
        there = number if arriving else grps - 2 - number
        return pltpu.make_async_remote_copy(
            src_ref=spot,
            dst_ref=spot,
            send_sem=y_send.at[piece],
            recv_sem=y_recv.at[piece, plane, there],
            device_id={"grp": other_grps[number]},
            device_id_type=MESH,
        )

    def send_own(piece, early=None):
        low, high = ends(piece)
        up, down = f < high, f > low
        if pieces[piece][0] > 2:
            outward_up, outward_down = f >= planes // 2, f < planes // 2
            up = up & (outward_up if early else jnp.logical_not(outward_up))
            down = down & (outward_down if early else jnp.logical_not(outward_down))

        @pl.when(up)
        def _():
            z_copy(piece, f, 1, own=True).start()

        @pl.when(down)
        def _():
            z_copy(piece, f, -1, own=True).start()

    def take(piece, hop):
        low, high = ends(piece)

        @pl.when((f >= hop) & (f <= high))
        def _():
            z_copy(piece, f - hop, -1).wait_recv()

            @pl.when(f < high)
            def _():
                z_copy(piece, f - hop, 1).start()

            @pl.when(wanted(piece))
            def _():
                for number in range(len(other_grps)):
                    y_copy(piece, f - hop, number, g).start()

        @pl.when((f + hop < planes) & (f >= low))
        def _():
            z_copy(piece, f + hop, 1).wait_recv()

            @pl.when(f > low)
            def _():
                z_copy(piece, f + hop, -1).start()

            @pl.when(wanted(piece))
            def _():
                for number in range(len(other_grps)):
                    y_copy(piece, f + hop, number, g).start()

    def advance(until):
        while clock[0] < until:
            step = clock[0]
            if step + ahead < len(pieces):
                send_own(step + ahead)
            if step in early_at:
                send_own(early_at[step], early=True)
            for hop in range(planes - 1, 0, -1):
                piece = step - (hop - 1) * lag
                if 0 <= piece < len(pieces):
                    take(piece, hop)
            clock[0] += 1

    def after(piece):
        return piece + 1 + (planes - 2) * lag

    def sent(piece):
        low, high = ends(piece)

        @pl.when(f < high)
        def _():
            z_copy(piece, f, 1, own=True).wait_send()

        @pl.when(f > low)
        def _():
            z_copy(piece, f, -1, own=True).wait_send()

        for hop in range(1, planes):

            @pl.when((f >= hop) & (f <= high))
            def _():
                @pl.when(f < high)
                def _():
                    z_copy(piece, f - hop, 1).wait_send()

                @pl.when(wanted(piece))
                def _():
                    for number in range(len(other_grps)):
                        y_copy(piece, f - hop, number, g).wait_send()

            @pl.when((f + hop < planes) & (f >= low))
            def _():
                @pl.when(f > low)
                def _():
                    z_copy(piece, f + hop, -1).wait_send()

                @pl.when(wanted(piece))
                def _():
                    for number in range(len(other_grps)):
                        y_copy(piece, f + hop, number, g).wait_send()

    def of(*numbers):
        return [p for p, piece in enumerate(pieces) if piece[0] in numbers]

    clock = [0]
    ahead = 2
    mixer_pieces = of(3, 4, 5)
    early_at = {8 * mixer_pieces[0] // 24 + i: p for i, p in enumerate(mixer_pieces)}
    lag = 1

    def arrive(*numbers):
        for number in numbers:
            local_copy(number).wait()
        for piece in of(*numbers):

            @pl.when(wanted(piece))
            def _():
                for step in range(1, planes):
                    plane = (f + step) % planes
                    for number, other in enumerate(other_grps):
                        y_copy(piece, plane, number, other, arriving=True).wait_recv()

    def local_copy(number):
        shard, whole, kind = weights[number]
        tall = shard.shape[0]
        span = pl.ds(pl.multiple_of(f * tall, 16), tall)
        if kind == "columns":
            mine = pl.ds(pl.multiple_of(side * share_units, 128), share_units)
            shard, spot = shard.at[:, mine], whole.at[side, span, :]
        elif kind == "rows":
            mine = pl.ds(pl.multiple_of(side * share_units, 16), share_units)
            shard, spot = shard.at[mine, :], whole.at[f, mine, :]
        elif kind == "stacked":
            spot = whole.at[f]
        else:
            spot = whole.at[span, :]
        return pltpu.make_async_copy(shard, spot, local_sem.at[number])

    def local_input():
        return pltpu.make_async_copy(inputs, input_all.at[tp], local_sem.at[len(weights)])

    row_tile = [t for t in (96, 64, 32, 16) if rows % t == 0][0]

    def spread(lane, half, with_mate=False):
        for peer in peers:
            value_copy(lane, tp, half, peer).start()
        if with_mate and mates > 1:
            value_copy(lane, tp, half).start()

    def landed(lane, block, half):
        value_copy(lane, block, half, partner).wait_recv()

    def relay_values(lane, half, with_mate=False):
        for twin in twins:
            landed(lane, twin, half)
            value_copy(lane, twin, half, partner, source=lane).start()
            if with_mate and mates > 1 and half == 1:
                value_copy(lane, twin, half, source=lane).start()

    def relay_mate(lane, half):
        landed(lane, tp, half)
        for peer in peers if half == 0 else [partner]:
            value_copy(lane, tp, half, peer, source=lane).start()

    def relay_mate_twins(lane):
        for half in range(2):
            for twin in twins:
                landed(lane, twin, half)
                value_copy(lane, twin, half, partner, source=lane).start()

    def gather_start(lane):
        for half in range(2):
            spread(lane, half, with_mate=True)

    def gather_relay(lane, mate_lane):
        relay_values(lane, 0)
        if mates > 1:
            relay_mate(mate_lane, 0)
        relay_values(lane, 1, with_mate=True)
        if mates > 1:
            relay_mate(mate_lane, 1)

    def value_sent(lane, with_mate=False):
        for half in range(2):
            for peer in peers:
                value_copy(lane, tp, half, peer).wait_send()
            for twin in twins:
                value_copy(lane, twin, half, partner, source=lane).wait_send()
            if with_mate and mates > 1:
                value_copy(lane, tp, half).wait_send()
                if half == 1:
                    for twin in twins:
                        value_copy(lane, twin, half, source=lane).wait_send()

    def mate_sent(lane):
        for half in range(2):
            for peer in peers if half == 0 else [partner]:
                value_copy(lane, tp, half, peer, source=lane).wait_send()
            for twin in twins:
                value_copy(lane, twin, half, partner, source=lane).wait_send()

    def scale_values(lane, slot, gain):
        for half in range(2):
            for block in [partner] + crosses:
                landed(lane, block, half)
        ref = gathered(lane)

        def body(step, carry):
            start = pl.multiple_of(step * row_tile, row_tile)
            span = pl.ds(start, row_tile)
            target = pl.ds(slot * rows + start, row_tile)
            total = jnp.zeros((row_tile, 1), F32)
            for t in range(tps):
                gains = gain_all[t].astype(F32)
                value = ref[t, span, :].astype(F32)
                total = total + jnp.sum(value * value, axis=1, keepdims=True)
                scaled[target, t * width : (t + 1) * width] = (
                    value * gains[gain : gain + 1]
                ).astype(BF16)
            factor[target, :] = lax.rsqrt(total / (tps * width) + 1e-06)
            return carry

        lax.fori_loop(0, rows // row_tile, body, 0)

    def hidden_units(slot):
        units = hidden.shape[1]
        tile = 256 if units % 256 == 0 else 128
        mine = slice(slot * rows, (slot + 1) * rows)

        def body(step, carry):
            span = pl.ds(pl.multiple_of(step * tile, tile), tile)
            gate = factor[mine, :] * jnp.dot(
                scaled[mine, :], gate_all[side, :, span], preferred_element_type=F32
            )
            up = factor[mine, :] * jnp.dot(
                scaled[mine, :], up_all[side, :, span], preferred_element_type=F32
            )
            hidden[mine, span] = (jax.nn.silu(gate) * up).astype(BF16)
            return carry

        lax.fori_loop(0, units // tile, body, 0)

    ratio = planes // tps
    block_width = width // ratio

    def product(left, right_of, lane, slot, block_of):
        for piece in range(ratio):
            parts[lane, block_of, :, piece * block_width : (piece + 1) * block_width] = jnp.dot(
                left[slot * rows : (slot + 1) * rows, :],
                right_of(block_of * ratio + piece),
                preferred_element_type=F32,
            ).astype(BF16)

    def join_cross(lane, twin, cross):
        sum_copy(lane, cross, cross, partner).wait_recv()
        parts[lane, twin] = (
            parts[lane, twin].astype(F32) + sums[lane, cross].astype(F32)
        ).astype(BF16)

    def project_mixer(lane):
        left, right_of = pooled, lambda plane: mout_all[plane]
        for twin, cross in zip(twins, crosses):
            product(left, right_of, lane, 0, cross)
            sum_copy(lane, cross, twin, partner).start()
        for twin, cross in zip(twins, crosses):
            product(left, right_of, lane, 0, twin)
            join_cross(lane, twin, cross)
            for half in range(2):
                sum_copy(lane, twin, tp, twin, half).start()
        product(left, right_of, lane, 0, partner)
        sum_copy(lane, partner, tp, partner).start()
        product(left, right_of, lane, 0, tp)

    def sum_sent(lane, half_only=None):
        for block in crosses + [partner]:
            sum_copy(lane, block, tp, partner).wait_send()
        for twin in twins:
            for half in range(2) if half_only is None else [half_only]:
                sum_copy(lane, twin, tp, twin, half).wait_send()

    def down_of(plane):
        return down_all[plane, pl.ds(pl.multiple_of(side * share_units, 16), share_units), :]

    def ffn_lanes(ffn):
        return [ffn * (mates + 1) + slot for slot in range(mates)]

    def project_cross(ffn, slot):
        lane = ffn_lanes(ffn)[slot]
        for twin, cross in zip(twins, crosses):
            product(hidden, down_of, lane, slot, cross)
            sum_copy(lane, cross, twin, partner).start()

    def project_twin(ffn, slot):
        lane = ffn_lanes(ffn)[slot]
        for twin, cross in zip(twins, crosses):
            product(hidden, down_of, lane, slot, twin)
            join_cross(lane, twin, cross)
            if slot > 0:
                mate_sum_copy(ffn, twin).start()
            sum_copy(lane, twin, tp, twin, 0).start()
            if mates == 1:
                sum_copy(lane, twin, tp, twin, 1).start()

    def project_partner(ffn, slot):
        lane = ffn_lanes(ffn)[slot]
        product(hidden, down_of, lane, slot, partner)
        sum_copy(lane, partner, tp, partner).start()

    def project_own(ffn, slot):
        product(hidden, down_of, ffn_lanes(ffn)[slot], slot, tp)

    def project_ffn(ffn):
        for stage in (project_cross, project_twin, project_partner, project_own):
            for slot in range(mates - 1, -1, -1):
                stage(ffn, slot)

    def half_total(lane, half, joined=False):
        total = parts[lane, tp, halves[half], :].astype(F32)
        if not joined:
            total = total + sums[lane, partner, halves[half], :].astype(F32)
        return total

    def add_twins(lane, half, total):
        for twin in twins:
            sum_copy(lane, twin, twin, partner, half).wait_recv()
            total = total + sums[lane, twin, halves[half], :].astype(F32)
        return total

    def exchange_ffn(ffn):
        lanes = ffn_lanes(ffn)
        if mates > 1:
            sum_copy(lanes[1], partner, partner, partner).wait_recv()
            mate_out[ffn, halves[1], :] = half_total(lanes[1], 1).astype(BF16)
            own_sum_copy(ffn).start()
            for twin in twins:
                mate_sum_copy(ffn, twin).wait_recv()
                parts[lanes[0], twin, halves[1], :] = (
                    parts[lanes[0], twin, halves[1], :].astype(F32)
                    + mate_in[ffn, twin].astype(F32)
                ).astype(BF16)
                sum_copy(lanes[0], twin, tp, twin, 1).start()
            mate_out[ffn, halves[0], :] = add_twins(
                lanes[1], 0, half_total(lanes[1], 0)
            ).astype(BF16)
            mate_sum_copy(ffn, tp, top=True).start()
        sum_copy(lanes[0], partner, partner, partner).wait_recv()

    def ffn_total(ffn, half):
        lane = ffn_lanes(ffn)[0]
        total = add_twins(lane, half, half_total(lane, half))
        if mates > 1 and half == 0:
            mate_sum_copy(ffn, tp, top=True).wait_recv()
            total = total + mate_top[ffn].astype(F32)
        elif mates > 1:
            own_sum_copy(ffn).wait_recv()
            total = total + mate_in[ffn, tp].astype(F32)
        return total

    def ffn_sent(ffn):
        lanes = ffn_lanes(ffn)
        sum_sent(lanes[0])
        if mates > 1:
            sum_sent(lanes[1], half_only=0)
            own_sum_copy(ffn).wait_send()
            mate_sum_copy(ffn, tp, top=True).wait_send()
            for twin in twins:
                mate_sum_copy(ffn, twin).wait_send()

    local_input().start()
    row = lax.broadcasted_iota(jnp.int32, (GAIN_ROWS, width), 0)
    gains = [ref[...].astype(F32) for ref in (first_gain, mixer_gain, second_gain)]
    gain_all[tp] = jnp.where(
        row == 0, gains[0], jnp.where(row == 1, gains[1], gains[2])
    ).astype(BF16)
    for half in range(2):
        spread(0, half)
    for peer in peers:
        gain_copy(tp, peer).start()
    for piece in range(ahead):
        send_own(piece)
    for number in range(len(weights)):
        local_copy(number).start()
    with scope("begin"):
        advance(1)
    local_input().wait()
    with scope("input_own"):
        for twin in twins:
            gain_copy(twin, partner).wait_recv()
            gain_copy(twin, partner, relay=True).start()
        for block in [partner] + crosses:
            gain_copy(block, partner).wait_recv()
        for half in range(2):
            relay_values(0, half)
        scale_values(0, 0, 0)
    with scope("early"):
        if mates > 1:
            value_copy(0, tp, 0).start()
        advance(2)
        if mates > 1:
            value_copy(0, tp, 1).start()
        advance(4)
    with scope("input_mate"):
        if mates > 1:
            for twin in twins:
                value_copy(0, twin, 1, source=0).start()
            relay_mate(3, 0)
            relay_mate(3, 1)
        advance(6)
        if mates > 1:
            relay_mate_twins(3)
    with scope("early2"):
        advance(7)
    with scope("mate_scale"):
        if mates > 1:
            scale_values(3, 1, 0)
    first_last, down_last = of(0, 1)[-1], of(2)[-1]
    with scope("gate_up"):
        advance(after(first_last) + 2)
    with scope("gate_up_y"):
        arrive(0, 1)
    for slot in range(mates):
        with scope(f"hidden{slot}"):
            hidden_units(slot)
        with scope(f"step{slot}"):
            advance(min(clock[0] + 2, after(down_last)))
    with scope("down"):
        advance(after(down_last))
    with scope("down_y"):
        arrive(2)
    with scope("project0"):
        project_ffn(0)
    with scope("mix_pool"):
        advance(after(of(3)[-1]))
    with scope("exchange0"):
        exchange_ffn(0)
    with scope("mix_gate"):
        advance(after(of(4)[0]))
    with scope("first"):
        for half, span in enumerate(halves):
            value_all[0, tp, span, :] = (
                input_all[tp, span, :].astype(F32) + 0.5 * ffn_total(0, half)
            ).astype(BF16)
            spread(1, half)
    with scope("mix_rest"):
        advance(after(len(pieces) - 1))
    with scope("sent1"):
        value_sent(0, with_mate=True)
        for peer in peers:
            gain_copy(tp, peer).wait_send()
        for twin in twins:
            gain_copy(twin, partner, relay=True).wait_send()
        if mates > 1:
            mate_sent(3)
        for piece in of(0):
            sent(piece)
    with scope("relay1"):
        for half in range(2):
            relay_values(1, half)
    with scope("scale1"):
        scale_values(1, 0, 1)
    with scope("mix_y"):
        arrive(3, 4)
    groups, group_width = mix_w.shape[0], mix_w.shape[1]
    with scope("pool"):
        mixed_rows = slice(0, rows)
        pool_pre = (
            factor[mixed_rows, :]
            * jnp.dot(scaled[mixed_rows, :], pool_all[...], preferred_element_type=F32)
        ).astype(BF16)
        position = lax.broadcasted_iota(jnp.int32, (rows, group_width), 0)
        for group in range(groups):
            span = slice(group * group_width, (group + 1) * group_width)
            value = pool_pre[:, span].astype(F32)
            kind = (tp * groups + group) % 4
            running = value
            chosen = jnp.zeros_like(value)
            for level in range(4):
                lag = 2**level
                running = running + jnp.where(
                    position >= lag, pltpu.roll(running, lag, axis=0), 0.0
                )
                counts = jnp.minimum(position + 1, 2 * lag).astype(F32)
                chosen = jnp.where(kind == level, running / counts, chosen)
            trail = (chosen - value).astype(BF16)
            mixed = jnp.dot(trail, mix_w[group], preferred_element_type=F32)
            pooled[:, span] = (mixed * scale_w[:, span]).astype(BF16)
    with scope("mix_y2"):
        arrive(5)
    with scope("project1"):
        project_mixer(mates)
    with scope("logit"):
        logit[...] = factor[mixed_rows, :] * jnp.dot(
            scaled[mixed_rows, :], mgate_all[...], preferred_element_type=F32
        )
        logit[...] = jax.nn.sigmoid(logit[...])
    with scope("sent2"):
        ffn_sent(0)
        value_sent(1)
    with scope("second"):
        sum_copy(mates, partner, partner, partner).wait_recv()
        for half, span in enumerate(halves):
            value_all[1, tp, span, :] = (
                value_all[0, tp, span, :].astype(F32)
                + logit[span, :] * add_twins(mates, half, half_total(mates, half))
            ).astype(BF16)
            spread(2, half, with_mate=True)
    with scope("sent3"):
        for piece in of(1, 2):
            sent(piece)
    with scope("relay2"):
        gather_relay(2, 4)
    with scope("scale2"):
        scale_values(2, 0, 2)
    with scope("hidden2_0"):
        hidden_units(0)
    with scope("project2_0"):
        project_cross(1, 0)
        if mates > 1:
            relay_mate_twins(4)
        project_partner(1, 0)
        project_own(1, 0)
        project_twin(1, 0)
    if mates > 1:
        with scope("scale4"):
            scale_values(4, 1, 2)
        with scope("hidden2_1"):
            hidden_units(1)
        with scope("project2_1"):
            project_cross(1, 1)
            project_partner(1, 1)
            project_twin(1, 1)
            project_own(1, 1)
    with scope("exchange2"):
        exchange_ffn(1)
    with scope("sent4"):
        sum_sent(mates)
        value_sent(2, with_mate=True)
        if mates > 1:
            mate_sent(4)
        for piece in of(3, 4, 5):
            sent(piece)
    with scope("final"):
        for half, span in enumerate(halves):
            out[span, :] = (
                value_all[1, tp, span, :].astype(F32) + 0.5 * ffn_total(1, half)
            ).astype(BF16)
    with scope("sent5"):
        ffn_sent(1)


def per_device(
    grps,
    planes,
    tps,
    layer_input,
    first_gain,
    ffn_gate_w,
    ffn_up_w,
    ffn_down_w,
    mixer_gain,
    pool_in_w,
    mixer_gate_w,
    group_mix_w,
    pool_scale,
    mixer_out_w,
    second_gain,
):
    rows, width = layer_input.shape
    features = width * tps
    units = ffn_gate_w.shape[1]
    channels = pool_in_w.shape[1]
    mates = 2 if planes % 2 == 0 else 1
    fine = max(8 // planes, 1)
    wanted = (fine, fine, 2 * fine, max(fine // 2, 1), fine, max(fine // 2, 1))
    shards = (ffn_gate_w, ffn_up_w, ffn_down_w, pool_in_w, mixer_gate_w, mixer_out_w)
    talls = [shard.shape[0] // grps for shard in shards]
    talls[2] //= mates
    piece_counts = tuple(ceil_pieces(tall, count) for tall, count in zip(talls, wanted))
    n = mates * sum(piece_counts[:3]) + sum(piece_counts[3:])
    lanes = 2 * mates + 1
    dma = pltpu.SemaphoreType.DMA
    whole = pl.BlockSpec(memory_space=pltpu.VMEM)
    remote = pl.BlockSpec(memory_space=pl.ANY)
    return pl.pallas_call(
        functools.partial(layer_kernel, (grps, planes, tps, mates, piece_counts)),
        out_shape=jax.ShapeDtypeStruct((rows, width), BF16),
        in_specs=[remote] + [whole] * 3 + [remote] * 6 + [whole] * 2,
        out_specs=whole,
        scratch_shapes=[
            pltpu.VMEM((mates, features, units // mates), BF16),
            pltpu.VMEM((mates, features, units // mates), BF16),
            pltpu.VMEM((planes,) + ffn_down_w.shape, BF16),
            pltpu.VMEM((features, channels), BF16),
            pltpu.VMEM((features, width), BF16),
            pltpu.VMEM((planes,) + mixer_out_w.shape, BF16),
            pltpu.VMEM((tps, rows, width), BF16),
            pltpu.VMEM((tps, GAIN_ROWS, width), BF16),
            pltpu.VMEM((2 * mates, tps, rows, width), BF16),
            pltpu.VMEM((mates * rows, features), BF16),
            pltpu.VMEM((mates * rows, 1), F32),
            pltpu.VMEM((mates * rows, units // mates), BF16),
            pltpu.VMEM((rows, channels), BF16),
            pltpu.VMEM((rows, width), F32),
            pltpu.VMEM((lanes, tps, rows, width), BF16),
            pltpu.VMEM((lanes, tps, rows, width), BF16),
            pltpu.VMEM((2, rows, width), BF16),
            pltpu.VMEM((2, tps, rows // 2, width), BF16),
            pltpu.VMEM((2, rows // 2, width), BF16),
            dma((len(shards) + 1,)),
            dma((n, planes)),
            dma((n, planes, max(grps - 1, 1))),
            dma((n,)),
            dma((n,)),
            dma((5,)),
            dma((5,)),
            dma((5, 2, tps)),
            dma(()),
            dma((tps,)),
            dma((lanes,)),
            dma((lanes, 2, tps)),
            dma((2,)),
            dma((2, tps + 1)),
        ],
        compiler_params=pltpu.CompilerParams(
            collective_id=0, has_side_effects=True, vmem_limit_bytes=60 * 1024 * 1024
        ),
    )(layer_input, first_gain, mixer_gain, second_gain, *shards, group_mix_w, pool_scale)


def solution(mesh):
    return jax.shard_map(
        functools.partial(
            per_device, mesh.shape["grp"], mesh.shape["fs"], mesh.shape["tp"]
        ),
        mesh=mesh,
        in_specs=(
            P(("grp", "fs"), "tp"),
            P(None, "tp"),
            P("fs", "tp"),
            P("fs", "tp"),
            P("tp", "fs"),
            P(None, "tp"),
            P("fs", "tp"),
            P("fs", "tp"),
            P("tp", None, None),
            P(None, "tp"),
            P("tp", "fs"),
            P(None, "tp"),
        ),
        out_specs=P(("grp", "fs"), "tp"),
        check_vma=False,
    )
```

```python
import functools

import jax
import jax.numpy as jnp
from jax import lax
from jax.experimental import pallas as pl
from jax.experimental.pallas import tpu as pltpu
from jax.sharding import PartitionSpec as P

MESH = pl.DeviceIdType.MESH
F32 = jnp.float32
BF16 = jnp.bfloat16
scope = jax.named_scope
GAIN_ROWS = 16


def ceil_pieces(rows, wanted):
    while rows % (wanted * 16) != 0:
        wanted -= 1
    return wanted


def layer_kernel(
    sizes,
    inputs,
    first_gain,
    mixer_gain,
    second_gain,
    gate_w,
    up_w,
    down_w,
    pool_w,
    mgate_w,
    mout_w,
    mix_w,
    scale_w,
    out,
    gate_all,
    up_all,
    down_all,
    pool_all,
    mgate_all,
    mout_all,
    input_all,
    gain_all,
    value_all,
    scaled,
    factor,
    hidden,
    pooled,
    logit,
    parts,
    sums,
    mate_out,
    mate_in,
    mate_top,
    local_sem,
    z_recv,
    y_recv,
    z_send,
    y_send,
    v_send,
    v_relay,
    v_recv,
    g_send,
    g_recv,
    s_send,
    s_recv,
    m_send,
    m_recv,
):
    grps, planes, tps, mates, piece_counts = sizes
    g = lax.axis_index("grp")
    f = lax.axis_index("fs")
    tp = lax.axis_index("tp")
    rows, width = out.shape
    chips = tps // 2
    chip, core = tp // 2, tp % 2
    partner = chip * 2 + (core + 1) % 2
    twins = [((chip + i) % chips) * 2 + core for i in range(1, chips)]
    crosses = [((chip + i) % chips) * 2 + (core + 1) % 2 for i in range(1, chips)]
    peers = twins + [partner]
    other_grps = [(g + d) % grps for d in range(1, grps)]
    side = f % mates
    mate = f + 1 - 2 * side

    barrier = pltpu.get_barrier_semaphore()
    for peer in peers:
        pl.semaphore_signal(barrier, inc=1, device_id={"tp": peer}, device_id_type=MESH)
    for other in other_grps:
        pl.semaphore_signal(barrier, inc=1, device_id={"grp": other}, device_id_type=MESH)

    @pl.when(f > 0)
    def _():
        pl.semaphore_signal(barrier, inc=1, device_id={"fs": f - 1}, device_id_type=MESH)

    @pl.when(f < planes - 1)
    def _():
        pl.semaphore_signal(barrier, inc=1, device_id={"fs": f + 1}, device_id_type=MESH)

    inner = jnp.where(f > 0, 1, 0) + jnp.where(f < planes - 1, 1, 0)
    pl.semaphore_wait(barrier, len(peers) + len(other_grps) + inner)

    def gathered(lane):
        return input_all if lane == 0 else value_all.at[lane - 1]

    half_rows = rows // 2
    halves = (slice(0, half_rows), slice(half_rows, rows))

    def value_copy(lane, block, half, peer=None, source=None):
        relay = source is not None
        ref = inputs if lane == 0 and not relay else gathered(source if relay else lane).at[block]
        to = lane if peer is not None else lane + 3 if lane == 0 else 4
        return pltpu.make_async_remote_copy(
            src_ref=ref.at[halves[half], :],
            dst_ref=gathered(to).at[block, halves[half], :],
            send_sem=(v_relay if relay else v_send).at[lane],
            recv_sem=v_recv.at[to, half, block],
            device_id={"fs": mate} if peer is None else {"tp": peer},
            device_id_type=MESH,
        )

    def gain_copy(block, peer, relay=False):
        return pltpu.make_async_remote_copy(
            src_ref=gain_all.at[block],
            dst_ref=gain_all.at[block],
            send_sem=g_send,
            recv_sem=g_recv.at[block],
            device_id={"tp": peer},
            device_id_type=MESH,
        )

    def mate_sum_copy(ffn, block, top=False):
        if top:
            source, target = mate_out.at[ffn, halves[0], :], mate_top.at[ffn]
        else:
            target = mate_in.at[ffn, block]
            source = parts.at[ffn_lanes(ffn)[-1], block, halves[1], :]
        number = tps if top else block
        return pltpu.make_async_remote_copy(
            src_ref=source,
            dst_ref=target,
            send_sem=m_send.at[ffn],
            recv_sem=m_recv.at[ffn, number],
            device_id={"fs": mate},
            device_id_type=MESH,
        )

    def own_sum_copy(ffn):
        return pltpu.make_async_remote_copy(
            src_ref=mate_out.at[ffn, halves[1], :],
            dst_ref=mate_in.at[ffn, tp],
            send_sem=m_send.at[ffn],
            recv_sem=m_recv.at[ffn, tp],
            device_id={"fs": mate},
            device_id_type=MESH,
        )

    def sum_copy(lane, block, slot, peer, half=None):
        span = slice(0, rows) if half is None else halves[half]
        number = 0 if half is None else half
        return pltpu.make_async_remote_copy(
            src_ref=parts.at[lane, block, span, :],
            dst_ref=sums.at[lane, slot, span, :],
            send_sem=s_send.at[lane],
            recv_sem=s_recv.at[lane, number, slot],
            device_id={"tp": peer},
            device_id_type=MESH,
        )

    weights = (
        (gate_w, gate_all, "columns"),
        (up_w, up_all, "columns"),
        (down_w, down_all, "rows"),
        (pool_w, pool_all, "plain"),
        (mgate_w, mgate_all, "plain"),
        (mout_w, mout_all, "stacked"),
    )
    pieces = []
    for numbers in ((0, 1), (2,), (3,), (4,), (5,)):
        for part in range(piece_counts[numbers[0]]):
            for number in numbers:
                for share in range(mates) if number < 3 else (None,):
                    pieces.append((number, share, part))
    share_units = down_w.shape[0] // mates

    def span_of(piece, grp):
        number, share, part = pieces[piece]
        kind = weights[number][2]
        tall = share_units if kind == "rows" else weights[number][0].shape[0]
        half = tall // grps
        size = half // piece_counts[number]
        offset = share * share_units if kind == "rows" else 0
        return offset + grp * half + part * size, size

    def place(piece, plane, grp):
        number, share, part = pieces[piece]
        shard, whole, kind = weights[number]
        start, size = span_of(piece, grp)
        if kind in ("rows", "stacked"):
            return whole.at[plane, pl.ds(pl.multiple_of(start, 16), size), :]
        span = pl.ds(pl.multiple_of(plane * shard.shape[0] + start, 16), size)
        if kind == "columns":
            return whole.at[share, span, :]
        return whole.at[span, :]

    def own_place(piece):
        number, share, part = pieces[piece]
        shard, whole, kind = weights[number]
        start, size = span_of(piece, g)
        span = pl.ds(pl.multiple_of(start, 16), size)
        if kind == "columns":
            return shard.at[span, share * share_units : (share + 1) * share_units]
        return shard.at[span, :]

    def ends(piece):
        share = pieces[piece][1]
        if share is None:
            return 0, planes - 1
        return share, planes - mates + share

    def wanted(piece):
        share = pieces[piece][1]
        return True if share is None else side == share

    def z_copy(piece, plane, step, own=False):
        spot = place(piece, plane, g)
        return pltpu.make_async_remote_copy(
            src_ref=own_place(piece) if own else spot,
            dst_ref=spot,
            send_sem=z_send.at[piece],
            recv_sem=z_recv.at[piece, plane],
            device_id={"fs": f + step},
            device_id_type=MESH,
        )

    def y_copy(piece, plane, number, source, arriving=False):
        spot = place(piece, plane, source)
        there = number if arriving else grps - 2 - number
        return pltpu.make_async_remote_copy(
            src_ref=spot,
            dst_ref=spot,
            send_sem=y_send.at[piece],
            recv_sem=y_recv.at[piece, plane, there],
            device_id={"grp": other_grps[number]},
            device_id_type=MESH,
        )

    def send_own(piece, early=None):
        low, high = ends(piece)
        up, down = f < high, f > low
        if pieces[piece][0] > 2:
            outward_up, outward_down = f >= planes // 2, f < planes // 2
            up = up & (outward_up if early else jnp.logical_not(outward_up))
            down = down & (outward_down if early else jnp.logical_not(outward_down))

        @pl.when(up)
        def _():
            z_copy(piece, f, 1, own=True).start()

        @pl.when(down)
        def _():
            z_copy(piece, f, -1, own=True).start()

    def take(piece, hop):
        low, high = ends(piece)

        @pl.when((f >= hop) & (f <= high))
        def _():
            z_copy(piece, f - hop, -1).wait_recv()

            @pl.when(f < high)
            def _():
                z_copy(piece, f - hop, 1).start()

            @pl.when(wanted(piece))
            def _():
                for number in range(len(other_grps)):
                    y_copy(piece, f - hop, number, g).start()

        @pl.when((f + hop < planes) & (f >= low))
        def _():
            z_copy(piece, f + hop, 1).wait_recv()

            @pl.when(f > low)
            def _():
                z_copy(piece, f + hop, -1).start()

            @pl.when(wanted(piece))
            def _():
                for number in range(len(other_grps)):
                    y_copy(piece, f + hop, number, g).start()

    def advance(until):
        while clock[0] < until:
            step = clock[0]
            if step + ahead < len(pieces):
                send_own(step + ahead)
            if step in early_at:
                send_own(early_at[step], early=True)
            for hop in range(planes - 1, 0, -1):
                piece = step - (hop - 1) * lag
                if 0 <= piece < len(pieces):
                    take(piece, hop)
            clock[0] += 1

    def after(piece):
        return piece + 1 + (planes - 2) * lag

    def sent(piece):
        low, high = ends(piece)

        @pl.when(f < high)
        def _():
            z_copy(piece, f, 1, own=True).wait_send()

        @pl.when(f > low)
        def _():
            z_copy(piece, f, -1, own=True).wait_send()

        for hop in range(1, planes):

            @pl.when((f >= hop) & (f <= high))
            def _():
                @pl.when(f < high)
                def _():
                    z_copy(piece, f - hop, 1).wait_send()

                @pl.when(wanted(piece))
                def _():
                    for number in range(len(other_grps)):
                        y_copy(piece, f - hop, number, g).wait_send()

            @pl.when((f + hop < planes) & (f >= low))
            def _():
                @pl.when(f > low)
                def _():
                    z_copy(piece, f + hop, -1).wait_send()

                @pl.when(wanted(piece))
                def _():
                    for number in range(len(other_grps)):
                        y_copy(piece, f + hop, number, g).wait_send()

    def of(*numbers):
        return [p for p, piece in enumerate(pieces) if piece[0] in numbers]

    clock = [0]
    ahead = 2
    mixer_pieces = of(3, 4, 5)
    early_at = {8 * mixer_pieces[0] // 24 + i: p for i, p in enumerate(mixer_pieces)}
    lag = 1

    def arrive(*numbers):
        for number in numbers:
            local_copy(number).wait()
        for piece in of(*numbers):

            @pl.when(wanted(piece))
            def _():
                for step in range(1, planes):
                    plane = (f + step) % planes
                    for number, other in enumerate(other_grps):
                        y_copy(piece, plane, number, other, arriving=True).wait_recv()

    def local_copy(number):
        shard, whole, kind = weights[number]
        tall = shard.shape[0]
        span = pl.ds(pl.multiple_of(f * tall, 16), tall)
        if kind == "columns":
            mine = pl.ds(pl.multiple_of(side * share_units, 128), share_units)
            shard, spot = shard.at[:, mine], whole.at[side, span, :]
        elif kind == "rows":
            mine = pl.ds(pl.multiple_of(side * share_units, 16), share_units)
            shard, spot = shard.at[mine, :], whole.at[f, mine, :]
        elif kind == "stacked":
            spot = whole.at[f]
        else:
            spot = whole.at[span, :]
        return pltpu.make_async_copy(shard, spot, local_sem.at[number])

    def local_input():
        return pltpu.make_async_copy(inputs, input_all.at[tp], local_sem.at[len(weights)])

    row_tile = [t for t in (96, 64, 32, 16) if rows % t == 0][0]

    def spread(lane, half, with_mate=False):
        for peer in peers:
            value_copy(lane, tp, half, peer).start()
        if with_mate and mates > 1:
            value_copy(lane, tp, half).start()

    def landed(lane, block, half):
        value_copy(lane, block, half, partner).wait_recv()

    def relay_values(lane, half, with_mate=False):
        for twin in twins:
            landed(lane, twin, half)
            value_copy(lane, twin, half, partner, source=lane).start()
            if with_mate and mates > 1 and half == 1:
                value_copy(lane, twin, half, source=lane).start()

    def relay_mate(lane, half):
        landed(lane, tp, half)
        for peer in peers if half == 0 else [partner]:
            value_copy(lane, tp, half, peer, source=lane).start()

    def relay_mate_twins(lane):
        for half in range(2):
            for twin in twins:
                landed(lane, twin, half)
                value_copy(lane, twin, half, partner, source=lane).start()

    def gather_start(lane):
        for half in range(2):
            spread(lane, half, with_mate=True)

    def gather_relay(lane, mate_lane):
        relay_values(lane, 0)
        if mates > 1:
            relay_mate(mate_lane, 0)
        relay_values(lane, 1, with_mate=True)
        if mates > 1:
            relay_mate(mate_lane, 1)

    def value_sent(lane, with_mate=False):
        for half in range(2):
            for peer in peers:
                value_copy(lane, tp, half, peer).wait_send()
            for twin in twins:
                value_copy(lane, twin, half, partner, source=lane).wait_send()
            if with_mate and mates > 1:
                value_copy(lane, tp, half).wait_send()
                if half == 1:
                    for twin in twins:
                        value_copy(lane, twin, half, source=lane).wait_send()

    def mate_sent(lane):
        for half in range(2):
            for peer in peers if half == 0 else [partner]:
                value_copy(lane, tp, half, peer, source=lane).wait_send()
            for twin in twins:
                value_copy(lane, twin, half, partner, source=lane).wait_send()

    def scale_values(lane, slot, gain):
        for half in range(2):
            for block in [partner] + crosses:
                landed(lane, block, half)
        ref = gathered(lane)

        def body(step, carry):
            start = pl.multiple_of(step * row_tile, row_tile)
            span = pl.ds(start, row_tile)
            target = pl.ds(slot * rows + start, row_tile)
            total = jnp.zeros((row_tile, 1), F32)
            for t in range(tps):
                gains = gain_all[t].astype(F32)
                value = ref[t, span, :].astype(F32)
                total = total + jnp.sum(value * value, axis=1, keepdims=True)
                scaled[target, t * width : (t + 1) * width] = (
                    value * gains[gain : gain + 1]
                ).astype(BF16)
            factor[target, :] = lax.rsqrt(total / (tps * width) + 1e-06)
            return carry

        lax.fori_loop(0, rows // row_tile, body, 0)

    def hidden_units(slot):
        units = hidden.shape[1]
        tile = 256 if units % 256 == 0 else 128
        mine = slice(slot * rows, (slot + 1) * rows)

        def body(step, carry):
            span = pl.ds(pl.multiple_of(step * tile, tile), tile)
            gate = factor[mine, :] * jnp.dot(
                scaled[mine, :], gate_all[side, :, span], preferred_element_type=F32
            )
            up = factor[mine, :] * jnp.dot(
                scaled[mine, :], up_all[side, :, span], preferred_element_type=F32
            )
            hidden[mine, span] = (jax.nn.silu(gate) * up).astype(BF16)
            return carry

        lax.fori_loop(0, units // tile, body, 0)

    ratio = planes // tps
    block_width = width // ratio

    def product(left, right_of, lane, slot, block_of):
        for piece in range(ratio):
            parts[lane, block_of, :, piece * block_width : (piece + 1) * block_width] = jnp.dot(
                left[slot * rows : (slot + 1) * rows, :],
                right_of(block_of * ratio + piece),
                preferred_element_type=F32,
            ).astype(BF16)

    def join_cross(lane, twin, cross):
        sum_copy(lane, cross, cross, partner).wait_recv()
        parts[lane, twin] = (
            parts[lane, twin].astype(F32) + sums[lane, cross].astype(F32)
        ).astype(BF16)

    def project_mixer(lane):
        left, right_of = pooled, lambda plane: mout_all[plane]
        for twin, cross in zip(twins, crosses):
            product(left, right_of, lane, 0, cross)
            sum_copy(lane, cross, twin, partner).start()
        for twin, cross in zip(twins, crosses):
            product(left, right_of, lane, 0, twin)
            join_cross(lane, twin, cross)
            for half in range(2):
                sum_copy(lane, twin, tp, twin, half).start()
        product(left, right_of, lane, 0, partner)
        sum_copy(lane, partner, tp, partner).start()
        product(left, right_of, lane, 0, tp)

    def sum_sent(lane, half_only=None):
        for block in crosses + [partner]:
            sum_copy(lane, block, tp, partner).wait_send()
        for twin in twins:
            for half in range(2) if half_only is None else [half_only]:
                sum_copy(lane, twin, tp, twin, half).wait_send()

    def down_of(plane):
        return down_all[plane, pl.ds(pl.multiple_of(side * share_units, 16), share_units), :]

    def ffn_lanes(ffn):
        return [ffn * (mates + 1) + slot for slot in range(mates)]

    def project_cross(ffn, slot):
        lane = ffn_lanes(ffn)[slot]
        for twin, cross in zip(twins, crosses):
            product(hidden, down_of, lane, slot, cross)
            sum_copy(lane, cross, twin, partner).start()

    def project_twin(ffn, slot):
        lane = ffn_lanes(ffn)[slot]
        for twin, cross in zip(twins, crosses):
            product(hidden, down_of, lane, slot, twin)
            join_cross(lane, twin, cross)
            if slot > 0 and ffn > 0:
                mate_sum_copy(ffn, twin).start()
            sum_copy(lane, twin, tp, twin, 0).start()
            if mates == 1 or ffn == 0:
                sum_copy(lane, twin, tp, twin, 1).start()

    def project_partner(ffn, slot):
        lane = ffn_lanes(ffn)[slot]
        product(hidden, down_of, lane, slot, partner)
        sum_copy(lane, partner, tp, partner).start()

    def project_own(ffn, slot):
        product(hidden, down_of, ffn_lanes(ffn)[slot], slot, tp)

    def project_ffn(ffn):
        for stage in (project_cross, project_twin, project_partner, project_own):
            for slot in range(mates - 1, -1, -1):
                stage(ffn, slot)

    def half_total(lane, half, joined=False):
        total = parts[lane, tp, halves[half], :].astype(F32)
        if not joined:
            total = total + sums[lane, partner, halves[half], :].astype(F32)
        return total

    def add_twins(lane, half, total):
        for twin in twins:
            sum_copy(lane, twin, twin, partner, half).wait_recv()
            total = total + sums[lane, twin, halves[half], :].astype(F32)
        return total

    def return_half(ffn, half):
        lane = ffn_lanes(ffn)[1]
        mate_out[ffn, halves[half], :] = add_twins(lane, half, half_total(lane, half)).astype(BF16)
        if half == 0:
            mate_sum_copy(ffn, tp, top=True).start()
        else:
            own_sum_copy(ffn).start()

    def partner_sums(ffn):
        for lane in ffn_lanes(ffn):
            sum_copy(lane, partner, partner, partner).wait_recv()

    def exchange_second():
        lanes = ffn_lanes(1)
        partner_sums(1)
        if mates > 1:
            mate_out[1, halves[1], :] = half_total(lanes[1], 1).astype(BF16)
            own_sum_copy(1).start()
            for twin in twins:
                mate_sum_copy(1, twin).wait_recv()
                parts[lanes[0], twin, halves[1], :] = (
                    parts[lanes[0], twin, halves[1], :].astype(F32)
                    + mate_in[1, twin].astype(F32)
                ).astype(BF16)
                sum_copy(lanes[0], twin, tp, twin, 1).start()
            return_half(1, 0)

    def ffn_total(ffn, half):
        lane = ffn_lanes(ffn)[0]
        total = add_twins(lane, half, half_total(lane, half))
        if mates > 1 and half == 0:
            mate_sum_copy(ffn, tp, top=True).wait_recv()
            total = total + mate_top[ffn].astype(F32)
        elif mates > 1:
            own_sum_copy(ffn).wait_recv()
            total = total + mate_in[ffn, tp].astype(F32)
        return total

    def ffn_sent(ffn):
        lanes = ffn_lanes(ffn)
        sum_sent(lanes[0])
        if mates > 1:
            sum_sent(lanes[1], half_only=0 if ffn else None)
            own_sum_copy(ffn).wait_send()
            mate_sum_copy(ffn, tp, top=True).wait_send()
            for twin in twins if ffn else []:
                mate_sum_copy(ffn, twin).wait_send()

    local_input().start()
    row = lax.broadcasted_iota(jnp.int32, (GAIN_ROWS, width), 0)
    gains = [ref[...].astype(F32) for ref in (first_gain, mixer_gain, second_gain)]
    gain_all[tp] = jnp.where(
        row == 0, gains[0], jnp.where(row == 1, gains[1], gains[2])
    ).astype(BF16)
    for half in range(2):
        spread(0, half)
    for peer in peers:
        gain_copy(tp, peer).start()
    for piece in range(ahead):
        send_own(piece)
    for number in range(len(weights)):
        local_copy(number).start()
    with scope("begin"):
        advance(1)
    local_input().wait()
    with scope("input_own"):
        for twin in twins:
            gain_copy(twin, partner).wait_recv()
            gain_copy(twin, partner, relay=True).start()
        for block in [partner] + crosses:
            gain_copy(block, partner).wait_recv()
        for half in range(2):
            relay_values(0, half)
        scale_values(0, 0, 0)
    with scope("early"):
        if mates > 1:
            value_copy(0, tp, 0).start()
        advance(2)
        if mates > 1:
            value_copy(0, tp, 1).start()
        advance(4)
    with scope("input_mate"):
        if mates > 1:
            for twin in twins:
                value_copy(0, twin, 1, source=0).start()
            relay_mate(3, 0)
            relay_mate(3, 1)
        advance(6)
        if mates > 1:
            relay_mate_twins(3)
    with scope("early2"):
        advance(7)
    with scope("mate_scale"):
        if mates > 1:
            scale_values(3, 1, 0)
    first_last, down_last = of(0, 1)[-1], of(2)[-1]
    with scope("gate_up"):
        advance(after(first_last) + 2)
    with scope("gate_up_y"):
        arrive(0, 1)
    for slot in range(mates):
        with scope(f"hidden{slot}"):
            hidden_units(slot)
        with scope(f"step{slot}"):
            advance(min(clock[0] + 2, after(down_last)))
    with scope("down"):
        advance(after(down_last))
    with scope("down_y"):
        arrive(2)
    with scope("project0"):
        project_ffn(0)
    done = after(len(pieces) - 1)
    for half in range(2):
        with scope(f"mix{half}"):
            advance(min(clock[0] + 1, done))
        with scope(f"exchange0_{half}"):
            if half == 0:
                partner_sums(0)
            if mates > 1:
                return_half(0, half)
    for half, span in enumerate(halves):
        with scope(f"mix{2 + half}"):
            if half == 1:
                advance(min(clock[0] + 1, done))
        with scope(f"first{half}"):
            value_all[0, tp, span, :] = (
                input_all[tp, span, :].astype(F32) + 0.5 * ffn_total(0, half)
            ).astype(BF16)
            spread(1, half)
    with scope("mix_rest"):
        advance(done)
    with scope("sent1"):
        value_sent(0, with_mate=True)
        for peer in peers:
            gain_copy(tp, peer).wait_send()
        for twin in twins:
            gain_copy(twin, partner, relay=True).wait_send()
        if mates > 1:
            mate_sent(3)
        for piece in of(0):
            sent(piece)
    with scope("relay1"):
        for half in range(2):
            relay_values(1, half)
    with scope("scale1"):
        scale_values(1, 0, 1)
    with scope("mix_y"):
        arrive(3, 4)
    groups, group_width = mix_w.shape[0], mix_w.shape[1]
    with scope("pool"):
        mixed_rows = slice(0, rows)
        pool_pre = (
            factor[mixed_rows, :]
            * jnp.dot(scaled[mixed_rows, :], pool_all[...], preferred_element_type=F32)
        ).astype(BF16)
        position = lax.broadcasted_iota(jnp.int32, (rows, group_width), 0)
        for group in range(groups):
            span = slice(group * group_width, (group + 1) * group_width)
            value = pool_pre[:, span].astype(F32)
            kind = (tp * groups + group) % 4
            running = value
            chosen = jnp.zeros_like(value)
            for level in range(4):
                lag = 2**level
                running = running + jnp.where(
                    position >= lag, pltpu.roll(running, lag, axis=0), 0.0
                )
                counts = jnp.minimum(position + 1, 2 * lag).astype(F32)
                chosen = jnp.where(kind == level, running / counts, chosen)
            trail = (chosen - value).astype(BF16)
            mixed = jnp.dot(trail, mix_w[group], preferred_element_type=F32)
            pooled[:, span] = (mixed * scale_w[:, span]).astype(BF16)
    with scope("mix_y2"):
        arrive(5)
    with scope("project1"):
        project_mixer(mates)
    with scope("logit"):
        logit[...] = factor[mixed_rows, :] * jnp.dot(
            scaled[mixed_rows, :], mgate_all[...], preferred_element_type=F32
        )
        logit[...] = jax.nn.sigmoid(logit[...])
    with scope("sent2"):
        ffn_sent(0)
        value_sent(1)
    with scope("second"):
        sum_copy(mates, partner, partner, partner).wait_recv()
        for half, span in enumerate(halves):
            value_all[1, tp, span, :] = (
                value_all[0, tp, span, :].astype(F32)
                + logit[span, :] * add_twins(mates, half, half_total(mates, half))
            ).astype(BF16)
            spread(2, half, with_mate=True)
    with scope("sent3"):
        for piece in of(1, 2):
            sent(piece)
    with scope("relay2"):
        gather_relay(2, 4)
    with scope("scale2"):
        scale_values(2, 0, 2)
    with scope("hidden2_0"):
        hidden_units(0)
    with scope("project2_0"):
        project_cross(1, 0)
        if mates > 1:
            relay_mate_twins(4)
        project_partner(1, 0)
        project_own(1, 0)
        project_twin(1, 0)
    if mates > 1:
        with scope("scale4"):
            scale_values(4, 1, 2)
        with scope("hidden2_1"):
            hidden_units(1)
        with scope("project2_1"):
            project_cross(1, 1)
            project_partner(1, 1)
            project_twin(1, 1)
            project_own(1, 1)
    with scope("exchange2"):
        exchange_second()
    with scope("sent4"):
        sum_sent(mates)
        value_sent(2, with_mate=True)
        if mates > 1:
            mate_sent(4)
        for piece in of(3, 4, 5):
            sent(piece)
    with scope("final"):
        for half, span in enumerate(halves):
            out[span, :] = (
                value_all[1, tp, span, :].astype(F32) + 0.5 * ffn_total(1, half)
            ).astype(BF16)
    with scope("sent5"):
        ffn_sent(1)


def per_device(
    grps,
    planes,
    tps,
    layer_input,
    first_gain,
    ffn_gate_w,
    ffn_up_w,
    ffn_down_w,
    mixer_gain,
    pool_in_w,
    mixer_gate_w,
    group_mix_w,
    pool_scale,
    mixer_out_w,
    second_gain,
):
    rows, width = layer_input.shape
    features = width * tps
    units = ffn_gate_w.shape[1]
    channels = pool_in_w.shape[1]
    mates = 2 if planes % 2 == 0 else 1
    fine = max(8 // planes, 1)
    wanted = (fine, fine, 2 * fine, max(fine // 2, 1), fine, max(fine // 2, 1))
    shards = (ffn_gate_w, ffn_up_w, ffn_down_w, pool_in_w, mixer_gate_w, mixer_out_w)
    talls = [shard.shape[0] // grps for shard in shards]
    talls[2] //= mates
    piece_counts = tuple(ceil_pieces(tall, count) for tall, count in zip(talls, wanted))
    n = mates * sum(piece_counts[:3]) + sum(piece_counts[3:])
    lanes = 2 * mates + 1
    dma = pltpu.SemaphoreType.DMA
    whole = pl.BlockSpec(memory_space=pltpu.VMEM)
    remote = pl.BlockSpec(memory_space=pl.ANY)
    return pl.pallas_call(
        functools.partial(layer_kernel, (grps, planes, tps, mates, piece_counts)),
        out_shape=jax.ShapeDtypeStruct((rows, width), BF16),
        in_specs=[remote] + [whole] * 3 + [remote] * 6 + [whole] * 2,
        out_specs=whole,
        scratch_shapes=[
            pltpu.VMEM((mates, features, units // mates), BF16),
            pltpu.VMEM((mates, features, units // mates), BF16),
            pltpu.VMEM((planes,) + ffn_down_w.shape, BF16),
            pltpu.VMEM((features, channels), BF16),
            pltpu.VMEM((features, width), BF16),
            pltpu.VMEM((planes,) + mixer_out_w.shape, BF16),
            pltpu.VMEM((tps, rows, width), BF16),
            pltpu.VMEM((tps, GAIN_ROWS, width), BF16),
            pltpu.VMEM((2 * mates, tps, rows, width), BF16),
            pltpu.VMEM((mates * rows, features), BF16),
            pltpu.VMEM((mates * rows, 1), F32),
            pltpu.VMEM((mates * rows, units // mates), BF16),
            pltpu.VMEM((rows, channels), BF16),
            pltpu.VMEM((rows, width), F32),
            pltpu.VMEM((lanes, tps, rows, width), BF16),
            pltpu.VMEM((lanes, tps, rows, width), BF16),
            pltpu.VMEM((2, rows, width), BF16),
            pltpu.VMEM((2, tps, rows // 2, width), BF16),
            pltpu.VMEM((2, rows // 2, width), BF16),
            dma((len(shards) + 1,)),
            dma((n, planes)),
            dma((n, planes, max(grps - 1, 1))),
            dma((n,)),
            dma((n,)),
            dma((5,)),
            dma((5,)),
            dma((5, 2, tps)),
            dma(()),
            dma((tps,)),
            dma((lanes,)),
            dma((lanes, 2, tps)),
            dma((2,)),
            dma((2, tps + 1)),
        ],
        compiler_params=pltpu.CompilerParams(
            collective_id=0, has_side_effects=True, vmem_limit_bytes=60 * 1024 * 1024
        ),
    )(layer_input, first_gain, mixer_gain, second_gain, *shards, group_mix_w, pool_scale)


def solution(mesh):
    return jax.shard_map(
        functools.partial(
            per_device, mesh.shape["grp"], mesh.shape["fs"], mesh.shape["tp"]
        ),
        mesh=mesh,
        in_specs=(
            P(("grp", "fs"), "tp"),
            P(None, "tp"),
            P("fs", "tp"),
            P("fs", "tp"),
            P("tp", "fs"),
            P(None, "tp"),
            P("fs", "tp"),
            P("fs", "tp"),
            P("tp", None, None),
            P(None, "tp"),
            P("tp", "fs"),
            P(None, "tp"),
        ),
        out_specs=P(("grp", "fs"), "tp"),
        check_vma=False,
    )
```
